32 devices in a mesh: ra: 4 (over z), cb: 4 (over y, x), dp: 2 (over core).
Axes of the slice: x: 2, y: 2, z: 4, core: 2. Of those that a mesh axis runs over, the one named last changes fastest.
Arguments:
- tokens: bfloat16 [2, 512, 4096], P('dp', None, 'ra'), may hold values from -80 to 80
- pre_gain: float32 [4096], P('ra'), may hold values from 0.1 to 1.9
- w_gate: bfloat16 [4096, 11264], P('ra', 'cb'), may hold values from -0.09375 to 0.09375
- w_up: bfloat16 [4096, 11264], P('ra', 'cb'), may hold values from -0.09375 to 0.09375
- conv_gate: float32 [3, 11264], P(None, 'cb'), may hold values from -3.5 to 3.5
- conv_up: float32 [3, 11264], P(None, 'cb'), may hold values from -3.5 to 3.5
- w_down: bfloat16 [11264, 4096], P('cb', 'ra'), may hold values from -2 to 2
- post_gain: float32 [4096], P('ra'), may hold values from 0.1 to 1.9
Outputs:
- mixed: bfloat16 [2, 512, 4096], P('dp', None, 'ra')
The draws below stay inside these ranges and needn't reach their ends.
All inputs are finite; a program needn't handle non-finite values.
Results may differ from the reference program's by a relative error of at most 0.0064.
Values may be sent and summed in bfloat16 or wider, within the bound.
A program may use at most 128 MiB of HBM per device.

```python
import math
import jax
import jax.numpy as jnp
from jax import lax

D = 4096
FF = 11264
TOK_DEV = 512
SEQS = 2


def column_scales(key, width):
    column = jnp.arange(width, dtype=jnp.float32) / (width - 1)
    return 10.0 ** column * jax.random.uniform(key, (width,), jnp.float32, 0.7, 1.4) / 4.0


def draw_tokens(key, part):
    first, second, third = jax.random.split(jax.random.fold_in(key, 11), 3)
    col_scale = column_scales(second, D)
    base = jnp.clip(jax.random.normal(first, (SEQS, TOK_DEV, D), jnp.float32), -6.0, 6.0)
    row_scale = jnp.exp(jax.random.uniform(third, (SEQS, TOK_DEV, 1), jnp.float32, 0.0, math.log(10.0)))
    return (base * row_scale * col_scale / 3.0).astype(jnp.bfloat16)


def draw_w_down(key, part):
    first, second = jax.random.split(jax.random.fold_in(key, 23), 2)
    col_scale = column_scales(second, D)
    base = jnp.clip(jax.random.normal(first, (FF, D), jnp.float32), -6.0, 6.0)
    return (base * col_scale / math.sqrt(FF)).astype(jnp.bfloat16)


def levels(key, extent, cuts, least, top_value):
    level = 1.0
    for axis_at, shards_of in cuts:
        draws = jax.random.uniform(jax.random.fold_in(jax.random.fold_in(key, 6), axis_at), (shards_of,), jnp.float32, least / len(cuts), top_value / len(cuts))
        level = level * jnp.repeat(jnp.exp(draws), extent[axis_at] // shards_of).reshape((-1,) + (1,) * (len(extent) - 1 - axis_at))
    return level


def normal_values(rng, dims, spread, reach, pieces=(), kind=jnp.bfloat16):
    gain = levels(rng, dims, pieces, -0.22, 0.18) if pieces else 1.0
    entries = jax.random.normal(rng, dims, jnp.float32) * spread * gain
    return jnp.minimum(jnp.maximum(entries, -reach), reach).astype(kind)


def setup_inputs(seed: int = 0) -> dict:
    key_list = jax.random.split(jax.random.key(seed), 9)
    return {
        "tokens": draw_tokens(jax.random.fold_in(key_list[8], 71), 0),
        "pre_gain": jnp.clip(1.0 + 0.18 * jax.random.normal(key_list[1], (D,), jnp.float32), 0.1, 1.9),
        "w_gate": normal_values(key_list[2], (D, FF), D ** -0.5, 0.09375, ((0, 4), (1, 4))),
        "w_up": normal_values(key_list[3], (D, FF), D ** -0.5, 0.09375, ((0, 4), (1, 4))),
        "conv_gate": normal_values(key_list[4], (3, FF), 3 ** -0.5, 3.5, ((1, 4),), jnp.float32),
        "conv_up": normal_values(key_list[5], (3, FF), 3 ** -0.5, 3.5, ((1, 4),), jnp.float32),
        "w_down": draw_w_down(jax.random.fold_in(key_list[8], 71), 0),
        "post_gain": jnp.clip(1.0 + 0.18 * jax.random.normal(key_list[7], (D,), jnp.float32), 0.1, 1.9),
    }


epsilon = 1e-06
residual_scale = 0.125

def shifted_sum(field, tap_weights):
    padded = jnp.pad(field, ((0, 0), (1, 1), (0, 0)))
    return padded[:, :-2] * tap_weights[0] + padded[:, 1:-1] * tap_weights[1] + padded[:, 2:] * tap_weights[2]

def reference(tokens, pre_gain, w_gate, w_up, conv_gate, conv_up, w_down, post_gain):
    seq_count, positions, features = tokens.shape
    values = tokens.astype(jnp.float32)
    pre_scale = lax.rsqrt(lax.optimization_barrier(jnp.mean(values * values, axis=-1, keepdims=True)) + epsilon)
    weighted = (values * pre_gain).astype(jnp.bfloat16).reshape(seq_count * positions, features)
    gate_lin = jnp.dot(weighted, w_gate, preferred_element_type=jnp.float32).reshape(seq_count, positions, -1) * pre_scale
    up_lin = jnp.dot(weighted, w_up, preferred_element_type=jnp.float32).reshape(seq_count, positions, -1) * pre_scale
    gate_conv = shifted_sum(gate_lin, conv_gate)
    up_conv = shifted_sum(up_lin, conv_up)
    hidden = (jax.nn.gelu(gate_conv, approximate=True) * up_conv).astype(jnp.bfloat16)
    branch = jnp.dot(hidden.reshape(seq_count * positions, -1), w_down, preferred_element_type=jnp.float32)
    branch = branch.reshape(seq_count, positions, features)
    post_scale = lax.rsqrt(lax.optimization_barrier(jnp.mean(branch * branch, axis=-1, keepdims=True)) + epsilon)
    mixed = residual_scale * values + branch * post_scale * post_gain
    return mixed.astype(jnp.bfloat16)
```

```python
import jax
import jax.numpy as jnp
from jax import lax
from jax.sharding import PartitionSpec as P

epsilon = 1e-06
residual_scale = 0.125


def convolve(field, tap_weights):
    zero_col = jnp.zeros((field.shape[0], 1), jnp.float32)
    before = jnp.concatenate([zero_col, field[:, :-1]], axis=1)
    later_cols = jnp.concatenate([field[:, 1:], zero_col], axis=1)
    return (
        tap_weights[0][:, None] * before
        + tap_weights[1][:, None] * field
        + tap_weights[2][:, None] * later_cols
    )


def local(tokens, pre_gain, w_gate, w_up, conv_gate, conv_up, w_down, post_gain):
    ra_count = lax.axis_size("ra")
    dim_full = tokens.shape[2] * ra_count
    values = tokens[0].astype(jnp.float32)
    local_sq = jnp.sum(values * values, axis=1)
    total_sq = lax.psum(local_sq, "ra")
    in_scale = lax.rsqrt(total_sq / dim_full + epsilon)
    weighted = (values * pre_gain).astype(jnp.bfloat16)
    wire = jnp.bfloat16 if ra_count <= 4 else jnp.float32
    dims = (((0,), (1,)), ((), ()))

    def summed(weights):
        part = lax.dot_general(weights, weighted, dims, preferred_element_type=jnp.float32)
        full = lax.psum_scatter(part.astype(wire), "ra", scatter_dimension=0, tiled=True)
        return full.astype(jnp.float32)

    gate_sum = summed(w_gate)
    up_sum = summed(w_up)
    own_units = gate_sum.shape[0]
    offset_units = lax.axis_index("ra") * own_units
    taps_gate = lax.dynamic_slice_in_dim(conv_gate, offset_units, own_units, 1)
    taps_up = lax.dynamic_slice_in_dim(conv_up, offset_units, own_units, 1)
    gate_lin = gate_sum * in_scale[None, :]
    up_lin = up_sum * in_scale[None, :]
    hidden = (
        jax.nn.gelu(convolve(gate_lin, taps_gate), approximate=True) * convolve(up_lin, taps_up)
    ).astype(jnp.bfloat16)
    partial_value = lax.dot_general(
        lax.all_gather(hidden, "ra", axis=0, tiled=True),
        w_down,
        (((0,), (0,)), ((), ())),
        preferred_element_type=jnp.float32,
    )
    branch = lax.psum_scatter(partial_value, "cb", scatter_dimension=0, tiled=True)
    rows = branch.shape[0]
    own = lax.dynamic_slice_in_dim(values, lax.axis_index("cb") * rows, rows, 0)
    post_sq = lax.psum(jnp.sum(branch * branch, axis=1), "ra")
    post_scale = lax.rsqrt(post_sq / dim_full + epsilon)
    mixed = residual_scale * own + branch * post_scale[:, None] * post_gain
    return lax.all_gather(mixed.astype(jnp.bfloat16), "cb", axis=0, tiled=True)[None]


def solution(mesh):
    in_specs = (
        P("dp", None, "ra"),
        P("ra"),
        P("ra", "cb"),
        P("ra", "cb"),
        P(None, "cb"),
        P(None, "cb"),
        P("cb", "ra"),
        P("ra"),
    )
    out_specs = P("dp", None, "ra")
    return jax.shard_map(local, mesh=mesh, in_specs=in_specs, out_specs=out_specs, check_vma=False)
```

```python
import functools
import jax
import jax.numpy as jnp
from jax import lax
from jax.experimental import pallas as pl
from jax.experimental.pallas import tpu as pltpu
from jax.sharding import PartitionSpec as P

epsilon = 1e-06
residual_scale = 0.125
LANES = 128
MESH = pl.DeviceIdType.MESH


def gelu(v):
    return 0.5 * v * (1.0 + jnp.tanh(0.7978845608028654 * (v + 0.044715 * v * v * v)))


def kernel(
    n, m, wire,
    tok_ref, pre_ref, wg_hbm, wu_hbm, cg_ref, cu_ref, wd_hbm, post_ref, out_ref,
    wg, wu, wd, xw, gu, rbuf, sbuf, hid, acc, sq_out, sq_in, scale, bsend, brecv, ps_out, ps_in,
    wsem, dsem, psend, precv, hsend, hrecv, sqs, sqr, bss, bsr, pss, psr, oss, osr,
):
    rows, width = tok_ref.shape
    chunks = rbuf.shape[1]
    half = chunks * LANES
    block = rows // m
    dim_full = width * n
    r = lax.axis_index("ra")
    me = lax.axis_index("cb")
    f32, bf16 = jnp.float32, jnp.bfloat16

    def units(d, c):
        return pl.ds(pl.multiple_of(d * half + c * LANES, LANES), LANES)

    def weight_copies(d, c):
        at = units(d, c)
        return (
            pltpu.make_async_copy(wg_hbm.at[:, at], wg.at[:, at], wsem.at[0, d, c]),
            pltpu.make_async_copy(wu_hbm.at[:, at], wu.at[:, at], wsem.at[1, d, c]),
        )

    first = (2 * r) // n

    def fetch(c, carry):
        for i in (0, 1):
            for copy in weight_copies((i + first) % 2, c):
                copy.start()
        return carry

    lax.fori_loop(0, chunks, fetch, 0)
    down_copy = pltpu.make_async_copy(wd_hbm, wd, dsem)
    down_copy.start()

    barrier = pltpu.get_barrier_semaphore()
    for k in range(1, n):
        pl.semaphore_signal(barrier, inc=1, device_id={"ra": (r + k) % n}, device_id_type=MESH)
    for k in range(1, m):
        pl.semaphore_signal(barrier, inc=1, device_id={"cb": (me + k) % m}, device_id_type=MESH)

    values = tok_ref[...].astype(f32)
    xw[...] = (values * pre_ref[...]).astype(bf16)
    square = values * values
    high = square.astype(bf16)
    low = (square - high.astype(f32)).astype(bf16)
    ones = jnp.ones((8, width), bf16)
    nt = (((1,), (1,)), ((), ()))
    sq_out[...] = lax.dot_general(ones, high, nt, preferred_element_type=f32) + lax.dot_general(
        ones, low, nt, preferred_element_type=f32
    )
    acc[...] = jnp.zeros_like(acc)
    pl.semaphore_wait(barrier, n - 1 + m - 1)

    def square_copy(end, k):
        return pltpu.make_async_remote_copy(
            src_ref=sq_out, dst_ref=sq_in.at[k],
            send_sem=sqs.at[end], recv_sem=sqr.at[k],
            device_id={"ra": end * (n - 1)}, device_id_type=MESH,
        )

    for end in (0, 1):
        @pl.when(r != end * (n - 1))
        def _():
            square_copy(end, r).start()

    def partial_copy(d, c):
        return pltpu.make_async_remote_copy(
            src_ref=sbuf.at[d, c], dst_ref=rbuf.at[d, c],
            send_sem=psend.at[d, c], recv_sem=precv.at[d, c],
            device_id={"ra": (r + 1 - 2 * d + n) % n}, device_id_type=MESH,
        )

    def hidden_copy(d, c):
        return pltpu.make_async_remote_copy(
            src_ref=hid.at[d, c], dst_ref=hid.at[d, c],
            send_sem=hsend.at[d, c], recv_sem=hrecv.at[d, c],
            device_id={"ra": (r - 1 + 2 * d + n) % n}, device_id_type=MESH,
        )

    def place(d):
        return r * (1 - d) + (n - 1 - r) * d

    def total_scale():
        total = sq_out[...]
        for k in range(n):
            @pl.when(r != k)
            def _():
                square_copy(0, k).wait_recv()
            total = total + jnp.where(r != k, sq_in[k], 0.0)
        inv = lax.rsqrt(total / dim_full + epsilon)
        scale[...] = jnp.concatenate([inv] * (LANES // 8), axis=0).T

    def convolve(field, taps_ref, at):
        spot = lax.broadcasted_iota(jnp.int32, field.shape, 0)
        before = jnp.where(spot == 0, 0.0, pltpu.roll(field, 1, 0))
        after = jnp.where(spot == rows - 1, 0.0, pltpu.roll(field, rows - 1, 0))
        return taps_ref[0:1, at] * before + taps_ref[1:2, at] * field + taps_ref[2:3, at] * after

    def step(s, carry):
        for i in (0, 1):
            d = (i + first) % 2
            p = place(d)
            c = s - p

            @pl.when((c >= 0) & (c < chunks))
            def _():
                at = units(d, c)
                for copy in weight_copies(d, c):
                    copy.wait()
                gu[:, :LANES] = jnp.dot(xw[...], wg[:, at], preferred_element_type=f32)
                gu[:, LANES:] = jnp.dot(xw[...], wu[:, at], preferred_element_type=f32)

                @pl.when(p == 0)
                def _():
                    sbuf[d, c] = gu[...].astype(wire)
                    partial_copy(d, c).start()

                @pl.when(p > 0)
                def _():
                    partial_copy(d, c).wait_recv()

                @pl.when((p > 0) & (p < n - 1))
                def _():
                    sbuf[d, c] = (gu[...] + rbuf[d, c].astype(f32)).astype(wire)
                    partial_copy(d, c).start()

                @pl.when(p == n - 1)
                def _():
                    @pl.when(c == 0)
                    def _():
                        total_scale()

                    by = scale[...]
                    gate_lin = (gu[:, :LANES] + rbuf[d, c, :, :LANES].astype(f32)) * by
                    up_lin = (gu[:, LANES:] + rbuf[d, c, :, LANES:].astype(f32)) * by
                    gate_conv = convolve(gate_lin, cg_ref, at)
                    up_conv = convolve(up_lin, cu_ref, at)
                    hid[d, c] = (gelu(gate_conv) * up_conv).astype(bf16)
                    hidden_copy(d, c).start()

        @pl.when(s == n - 1)
        def _():
            down_copy.wait()

        for i in (0, 1):
            d = (1 - i + first) % 2
            p = place(d)
            c = s - 2 * (n - 1) + p

            @pl.when((c >= 0) & (c < chunks))
            def _():
                @pl.when(p < n - 1)
                def _():
                    hidden_copy(d, c).wait_recv()

                @pl.when((p > 0) & (p < n - 1))
                def _():
                    hidden_copy(d, c).start()

                acc[...] += jnp.dot(hid[d, c], wd[units(d, c), :], preferred_element_type=f32)

        return carry

    lax.fori_loop(0, chunks + 2 * (n - 1), step, 0)

    bsend[...] = acc[...].astype(wire)

    def rows_of(j):
        return pl.ds(pl.multiple_of(j * block, block), block)

    def branch_copy(k):
        peer = (me + k) % m
        return pltpu.make_async_remote_copy(
            src_ref=bsend.at[rows_of(peer)], dst_ref=brecv.at[k],
            send_sem=bss.at[k], recv_sem=bsr.at[k],
            device_id={"cb": peer}, device_id_type=MESH,
        )

    for k in range(1, m):
        branch_copy(k).start()
    for k in range(1, m):
        branch_copy(k).wait_recv()
    mine = rows_of(me)
    branch = acc[mine, :]
    for k in range(1, m):
        branch = branch + brecv[k].astype(f32)
    acc[mine, :] = branch
    ps_out[...] = jnp.broadcast_to(jnp.sum(branch * branch, axis=1, keepdims=True), (block, LANES))

    def post_copy(k):
        return pltpu.make_async_remote_copy(
            src_ref=ps_out, dst_ref=ps_in.at[k],
            send_sem=pss.at[k], recv_sem=psr.at[k],
            device_id={"ra": (r + k) % n}, device_id_type=MESH,
        )

    for k in range(1, n):
        post_copy(k).start()

    for end in (0, 1):
        @pl.when(r != end * (n - 1))
        def _():
            square_copy(end, r).wait_send()


    def drain(c, carry):
        for d in (0, 1):
            p = place(d)

            @pl.when(p < n - 1)
            def _():
                partial_copy(d, c).wait_send()

            @pl.when(p > 0)
            def _():
                hidden_copy(d, c).wait_send()
        return carry

    lax.fori_loop(0, chunks, drain, 0)
    for k in range(1, m):
        branch_copy(k).wait_send()

    total = ps_out[...]
    for k in range(1, n):
        post_copy(k).wait_recv()
        total = total + ps_in[k]
    inv = lax.rsqrt(total[:, 0:1] / dim_full + epsilon)
    mixed = residual_scale * tok_ref[mine, :].astype(f32) + acc[mine, :] * inv * post_ref[...]
    out_ref[mine, :] = mixed.astype(bf16)

    def out_copy(k):
        return pltpu.make_async_remote_copy(
            src_ref=out_ref.at[mine], dst_ref=out_ref.at[mine],
            send_sem=oss.at[k], recv_sem=osr.at[k],
            device_id={"cb": (me + k) % m}, device_id_type=MESH,
        )

    for k in range(1, m):
        out_copy(k).start()
    for k in range(1, m):
        out_copy(k).wait()
    for k in range(1, n):
        post_copy(k).wait_send()


def local(n, m, tokens, pre_gain, w_gate, w_up, conv_gate, conv_up, w_down, post_gain):
    rows, width = tokens.shape[1:]
    total_units = w_gate.shape[1]
    chunks = total_units // (2 * LANES)
    block = rows // m
    wire = jnp.bfloat16 if n <= 4 else jnp.float32
    f32, bf16 = jnp.float32, jnp.bfloat16
    vmem = pl.BlockSpec(memory_space=pltpu.VMEM)
    hbm = pl.BlockSpec(memory_space=pl.ANY)
    dma = pltpu.SemaphoreType.DMA
    out = pl.pallas_call(
        functools.partial(kernel, n, m, wire),
        out_shape=jax.ShapeDtypeStruct((rows, width), bf16),
        in_specs=[vmem, vmem, hbm, hbm, vmem, vmem, hbm, vmem],
        out_specs=vmem,
        scratch_shapes=[
            pltpu.VMEM(w_gate.shape, bf16),
            pltpu.VMEM(w_up.shape, bf16),
            pltpu.VMEM(w_down.shape, bf16),
            pltpu.VMEM((rows, width), bf16),
            pltpu.VMEM((rows, 2 * LANES), f32),
            pltpu.VMEM((2, chunks, rows, 2 * LANES), wire),
            pltpu.VMEM((2, chunks, rows, 2 * LANES), wire),
            pltpu.VMEM((2, chunks, rows, LANES), bf16),
            pltpu.VMEM((rows, width), f32),
            pltpu.VMEM((8, rows), f32),
            pltpu.VMEM((n, 8, rows), f32),
            pltpu.VMEM((rows, LANES), f32),
            pltpu.VMEM((rows, width), wire),
            pltpu.VMEM((m, block, width), wire),
            pltpu.VMEM((block, LANES), f32),
            pltpu.VMEM((n, block, LANES), f32),
            dma((2, 2, chunks)), dma,
            dma((2, chunks)), dma((2, chunks)), dma((2, chunks)), dma((2, chunks)),
            dma((2,)), dma((n,)), dma((m,)), dma((m,)), dma((n,)), dma((n,)), dma((m,)), dma((m,)),
        ],
        compiler_params=pltpu.CompilerParams(
            collective_id=0, has_side_effects=True, vmem_limit_bytes=60 * 1024 * 1024
        ),
    )(tokens[0], pre_gain[None], w_gate, w_up, conv_gate, conv_up, w_down, post_gain[None])
    return out[None]


def solution(mesh):
    in_specs = (
        P("dp", None, "ra"),
        P("ra"),
        P("ra", "cb"),
        P("ra", "cb"),
        P(None, "cb"),
        P(None, "cb"),
        P("cb", "ra"),
        P("ra"),
    )
    out_specs = P("dp", None, "ra")
    return jax.shard_map(
        functools.partial(local, mesh.shape["ra"], mesh.shape["cb"]),
        mesh=mesh, in_specs=in_specs, out_specs=out_specs, check_vma=False,
    )
```

```python
import functools
import jax
import jax.numpy as jnp
from jax import lax
from jax.experimental import pallas as pl
from jax.experimental.pallas import tpu as pltpu
from jax.sharding import PartitionSpec as P

epsilon = 1e-06
residual_scale = 0.125
LANES = 128
HALO = 16
MESH = pl.DeviceIdType.MESH


def gelu(v):
    return 0.5 * v * (1.0 + jnp.tanh(0.7978845608028654 * (v + 0.044715 * v * v * v)))


def kernel(
    n, m, wire,
    tok_ref, pre_ref, wg_hbm, wu_hbm, cg_ref, cu_ref, wd_hbm, post_ref, out_ref,
    wg, wu, wd, xw, gu, rbuf, sbuf, hid, acc, sq_out, sq_in, scale, bsend, brecv, ps_out, ps_in,
    wsem, dsem, psend, precv, hsend, hrecv, sqs, sqr, bss, bsr, pss, psr, oss, osr,
):
    rows, width = tok_ref.shape
    chunks = rbuf.shape[1] // 2
    part = rows // 2
    span = part + HALO
    half = chunks * LANES
    block = part // m
    dim_full = width * n
    r = lax.axis_index("ra")
    me = lax.axis_index("cb")
    f32, bf16 = jnp.float32, jnp.bfloat16

    def units(d, c):
        return pl.ds(pl.multiple_of(d * half + c * LANES, LANES), LANES)

    def weight_copies(d, c):
        at = units(d, c)
        return (
            pltpu.make_async_copy(wg_hbm.at[:, at], wg.at[:, at], wsem.at[0, d, c]),
            pltpu.make_async_copy(wu_hbm.at[:, at], wu.at[:, at], wsem.at[1, d, c]),
        )

    first = (2 * r) // n

    def fetch(c, carry):
        for i in (0, 1):
            for copy in weight_copies((i + first) % 2, c):
                copy.start()
        return carry

    lax.fori_loop(0, chunks, fetch, 0)
    down_copy = pltpu.make_async_copy(wd_hbm, wd, dsem)
    down_copy.start()

    barrier = pltpu.get_barrier_semaphore()
    for k in range(1, n):
        pl.semaphore_signal(barrier, inc=1, device_id={"ra": (r + k) % n}, device_id_type=MESH)
    for k in range(1, m):
        pl.semaphore_signal(barrier, inc=1, device_id={"cb": (me + k) % m}, device_id_type=MESH)

    values = tok_ref[...].astype(f32)
    xw[...] = (values * pre_ref[...]).astype(bf16)
    square = values * values
    high = square.astype(bf16)
    low = (square - high.astype(f32)).astype(bf16)
    ones = jnp.ones((8, width), bf16)
    nt = (((1,), (1,)), ((), ()))
    sq_out[...] = lax.dot_general(ones, high, nt, preferred_element_type=f32) + lax.dot_general(
        ones, low, nt, preferred_element_type=f32
    )
    acc[...] = jnp.zeros_like(acc)
    pl.semaphore_wait(barrier, n - 1 + m - 1)

    def square_copy(end, k):
        return pltpu.make_async_remote_copy(
            src_ref=sq_out, dst_ref=sq_in.at[k],
            send_sem=sqs.at[end], recv_sem=sqr.at[k],
            device_id={"ra": end * (n - 1)}, device_id_type=MESH,
        )

    for end in (0, 1):
        @pl.when(r != end * (n - 1))
        def _():
            square_copy(end, r).start()

    def partial_copy(d, c):
        return pltpu.make_async_remote_copy(
            src_ref=sbuf.at[d, c], dst_ref=rbuf.at[d, c],
            send_sem=psend.at[d, c], recv_sem=precv.at[d, c],
            device_id={"ra": (r + 1 - 2 * d + n) % n}, device_id_type=MESH,
        )

    def hidden_copy(d, c):
        return pltpu.make_async_remote_copy(
            src_ref=hid.at[d, c, kept(c // chunks)], dst_ref=hid.at[d, c, kept(c // chunks)],
            send_sem=hsend.at[d, c], recv_sem=hrecv.at[d, c],
            device_id={"ra": (r - 1 + 2 * d + n) % n}, device_id_type=MESH,
        )

    def place(d):
        return r * (1 - d) + (n - 1 - r) * d

    def total_scale():
        total = sq_out[...]
        for k in range(n):
            @pl.when(r != k)
            def _():
                square_copy(0, k).wait_recv()
            total = total + jnp.where(r != k, sq_in[k], 0.0)
        inv = lax.rsqrt(total / dim_full + epsilon)
        scale[...] = jnp.concatenate([inv] * (LANES // 8), axis=0).T

    def taken(q):
        return pl.ds(pl.multiple_of(q * (part - HALO), HALO), span)

    def kept(q):
        return pl.ds(pl.multiple_of(q * HALO, HALO), part)

    def convolve(field, taps_ref, at, q):
        spot = lax.broadcasted_iota(jnp.int32, field.shape, 0) + q * (part - HALO)
        before = jnp.where(spot == 0, 0.0, pltpu.roll(field, 1, 0))
        after = jnp.where(spot == rows - 1, 0.0, pltpu.roll(field, span - 1, 0))
        return taps_ref[0:1, at] * before + taps_ref[1:2, at] * field + taps_ref[2:3, at] * after

    def step(s, carry):
        for i in (0, 1):
            d = (i + first) % 2
            p = place(d)
            c = s - p

            @pl.when((c >= 0) & (c < 2 * chunks))
            def _():
                q = c // chunks
                u = c % chunks
                at = units(d, u)

                @pl.when(q == 0)
                def _():
                    for copy in weight_copies(d, u):
                        copy.wait()

                gu[:, :LANES] = jnp.dot(xw[taken(q), :], wg[:, at], preferred_element_type=f32)
                gu[:, LANES:] = jnp.dot(xw[taken(q), :], wu[:, at], preferred_element_type=f32)

                @pl.when(p == 0)
                def _():
                    sbuf[d, c] = gu[...].astype(wire)
                    partial_copy(d, c).start()

                @pl.when(p > 0)
                def _():
                    partial_copy(d, c).wait_recv()

                @pl.when((p > 0) & (p < n - 1))
                def _():
                    sbuf[d, c] = (gu[...] + rbuf[d, c].astype(f32)).astype(wire)
                    partial_copy(d, c).start()

                @pl.when(p == n - 1)
                def _():
                    @pl.when(c == 0)
                    def _():
                        total_scale()

                    by = scale[taken(q), :]
                    gate_lin = (gu[:, :LANES] + rbuf[d, c, :, :LANES].astype(f32)) * by
                    up_lin = (gu[:, LANES:] + rbuf[d, c, :, LANES:].astype(f32)) * by
                    gate_conv = convolve(gate_lin, cg_ref, at, q)
                    up_conv = convolve(up_lin, cu_ref, at, q)
                    hid[d, c] = (gelu(gate_conv) * up_conv).astype(bf16)
                    hidden_copy(d, c).start()

        @pl.when(s == n - 1)
        def _():
            down_copy.wait()

        for i in (0, 1):
            d = (1 - i + first) % 2
            p = place(d)
            c = s - 2 * (n - 1) + p

            @pl.when((c >= 0) & (c < 2 * chunks))
            def _():
                q = c // chunks

                @pl.when(p < n - 1)
                def _():
                    hidden_copy(d, c).wait_recv()

                @pl.when((p > 0) & (p < n - 1))
                def _():
                    hidden_copy(d, c).start()

                at = pl.ds(pl.multiple_of(q * part, part), part)
                acc[at, :] += jnp.dot(
                    hid[d, c, kept(q), :], wd[units(d, c % chunks), :], preferred_element_type=f32
                )

        @pl.when(s == first_done)
        def _():
            send_branch(0)

        @pl.when(s == first_done + chunks // 3)
        def _():
            sum_branch(0)

        @pl.when(s == first_done + 2 * chunks // 3)
        def _():
            send_mixed(0)

        return carry

    first_done = chunks - 1 + 2 * (n - 1)

    def rows_of(q, j):
        return pl.ds(pl.multiple_of(q * part + j * block, block), block)

    def branch_copy(q, k):
        peer = (me + k) % m
        return pltpu.make_async_remote_copy(
            src_ref=bsend.at[rows_of(q, peer)], dst_ref=brecv.at[q, k],
            send_sem=bss.at[q, k], recv_sem=bsr.at[q, k],
            device_id={"cb": peer}, device_id_type=MESH,
        )

    def post_copy(q, k):
        return pltpu.make_async_remote_copy(
            src_ref=ps_out.at[q], dst_ref=ps_in.at[q, k],
            send_sem=pss.at[q, k], recv_sem=psr.at[q, k],
            device_id={"ra": (r + k) % n}, device_id_type=MESH,
        )

    def out_copy(q, k):
        mine = rows_of(q, me)
        return pltpu.make_async_remote_copy(
            src_ref=out_ref.at[mine], dst_ref=out_ref.at[mine],
            send_sem=oss.at[q, k], recv_sem=osr.at[q, k],
            device_id={"cb": (me + k) % m}, device_id_type=MESH,
        )

    def send_branch(q):
        at = pl.ds(q * part, part)
        bsend[at, :] = acc[at, :].astype(wire)
        for k in range(1, m):
            branch_copy(q, k).start()

    def sum_branch(q):
        mine = rows_of(q, me)
        branch = acc[mine, :]
        for k in range(1, m):
            branch_copy(q, k).wait_recv()
            branch = branch + brecv[q, k].astype(f32)
        acc[mine, :] = branch
        ps_out[q] = jnp.broadcast_to(jnp.sum(branch * branch, axis=1, keepdims=True), (block, LANES))
        for k in range(1, n):
            post_copy(q, k).start()

    def send_mixed(q):
        mine = rows_of(q, me)
        total = ps_out[q]
        for k in range(1, n):
            post_copy(q, k).wait_recv()
            total = total + ps_in[q, k]
        inv = lax.rsqrt(total[:, 0:1] / dim_full + epsilon)
        mixed = residual_scale * tok_ref[mine, :].astype(f32) + acc[mine, :] * inv * post_ref[...]
        out_ref[mine, :] = mixed.astype(bf16)
        for k in range(1, m):
            out_copy(q, k).start()

    lax.fori_loop(0, 2 * chunks + 2 * (n - 1), step, 0)
    send_branch(1)

    for end in (0, 1):
        @pl.when(r != end * (n - 1))
        def _():
            square_copy(end, r).wait_send()

    def drain(c, carry):
        for d in (0, 1):
            p = place(d)

            @pl.when(p < n - 1)
            def _():
                partial_copy(d, c).wait_send()

            @pl.when(p > 0)
            def _():
                hidden_copy(d, c).wait_send()
        return carry

    lax.fori_loop(0, 2 * chunks, drain, 0)
    sum_branch(1)
    send_mixed(1)
    for q in (0, 1):
        for k in range(1, m):
            branch_copy(q, k).wait_send()
            out_copy(q, k).wait()
        for k in range(1, n):
            post_copy(q, k).wait_send()


def local(n, m, tokens, pre_gain, w_gate, w_up, conv_gate, conv_up, w_down, post_gain):
    rows, width = tokens.shape[1:]
    total_units = w_gate.shape[1]
    chunks = total_units // (2 * LANES)
    block = rows // (2 * m)
    span = rows // 2 + HALO
    wire = jnp.bfloat16 if n <= 4 else jnp.float32
    f32, bf16 = jnp.float32, jnp.bfloat16
    vmem = pl.BlockSpec(memory_space=pltpu.VMEM)
    hbm = pl.BlockSpec(memory_space=pl.ANY)
    dma = pltpu.SemaphoreType.DMA
    out = pl.pallas_call(
        functools.partial(kernel, n, m, wire),
        out_shape=jax.ShapeDtypeStruct((rows, width), bf16),
        in_specs=[vmem, vmem, hbm, hbm, vmem, vmem, hbm, vmem],
        out_specs=vmem,
        scratch_shapes=[
            pltpu.VMEM(w_gate.shape, bf16),
            pltpu.VMEM(w_up.shape, bf16),
            pltpu.VMEM(w_down.shape, bf16),
            pltpu.VMEM((rows, width), bf16),
            pltpu.VMEM((span, 2 * LANES), f32),
            pltpu.VMEM((2, 2 * chunks, span, 2 * LANES), wire),
            pltpu.VMEM((2, 2 * chunks, span, 2 * LANES), wire),
            pltpu.VMEM((2, 2 * chunks, span, LANES), bf16),
            pltpu.VMEM((rows, width), f32),
            pltpu.VMEM((8, rows), f32),
            pltpu.VMEM((n, 8, rows), f32),
            pltpu.VMEM((rows, LANES), f32),
            pltpu.VMEM((rows, width), wire),
            pltpu.VMEM((2, m, block, width), wire),
            pltpu.VMEM((2, block, LANES), f32),
            pltpu.VMEM((2, n, block, LANES), f32),
            dma((2, 2, chunks)), dma,
            dma((2, 2 * chunks)), dma((2, 2 * chunks)), dma((2, 2 * chunks)), dma((2, 2 * chunks)),
            dma((2,)), dma((n,)), dma((2, m)), dma((2, m)), dma((2, n)), dma((2, n)), dma((2, m)), dma((2, m)),
        ],
        compiler_params=pltpu.CompilerParams(
            collective_id=0, has_side_effects=True, vmem_limit_bytes=60 * 1024 * 1024
        ),
    )(tokens[0], pre_gain[None], w_gate, w_up, conv_gate, conv_up, w_down, post_gain[None])
    return out[None]


def solution(mesh):
    in_specs = (
        P("dp", None, "ra"),
        P("ra"),
        P("ra", "cb"),
        P("ra", "cb"),
        P(None, "cb"),
        P(None, "cb"),
        P("cb", "ra"),
        P("ra"),
    )
    out_specs = P("dp", None, "ra")
    return jax.shard_map(
        functools.partial(local, mesh.shape["ra"], mesh.shape["cb"]),
        mesh=mesh, in_specs=in_specs, out_specs=out_specs, check_vma=False,
    )
```
